32 devices in a mesh: sp: 8 (over z, y), tp: 4 (over x, core).
Axes of the slice: x: 2, y: 2, z: 4, core: 2. Of those that a mesh axis runs over, the one named last changes fastest.
Arguments:
- latent: bfloat16 [4096, 4096], P(('sp', 'tp')), may hold values from -3 to 3
- context: bfloat16 [1024, 4096], P('sp'), may hold values from -6 to 6
- cond: float32 [4096], replicated, may hold values from -6 to 6
- ctx_cond: float32 [4096], replicated, may hold values from -6 to 6
- w_shift: bfloat16 [4096, 4096], P('sp', 'tp'), may hold values from -0.1875 to 0.1875
- w_scale: bfloat16 [4096, 4096], P('sp', 'tp'), may hold values from -0.09375 to 0.15478516
- w_gate: bfloat16 [4096, 4096], P('sp', 'tp'), may hold values from -0.1875 to 0.1875
- w_query: bfloat16 [4096, 2048], P(None, 'tp'), may hold values from -0.09375 to 0.09375
- key_weight: bfloat16 [4096, 1024], P(None, 'tp'), may hold values from -0.09375 to 0.09375
- value_weight: bfloat16 [4096, 1024], P(None, 'tp'), may hold values from -0.09375 to 0.09375
- w_out: bfloat16 [2048, 4096], P('tp'), may hold values from -0.125 to 0.125
- sink: float32 [16], replicated, may hold values from 4 to 8
Outputs:
- mixed: bfloat16 [4096, 4096], P(('sp', 'tp'))
The draws below stay inside these ranges and needn't reach their ends.
All inputs are finite; a program needn't handle non-finite values.
Results may differ from the reference program's by a relative error of at most 0.035.
Values may be sent and summed in bfloat16 or wider, within the bound.
A program may use at most 64 MiB of HBM per device.

```python
import math
import jax
import jax.numpy as jnp
from jax import lax

MODEL_WIDTH = 4096
HEAD_SIZE = 128
QUERY_HEADS = 16
KEY_VALUE_HEADS = 8
WINDOW_SIDE = 128
GRID_WIDTH = 64
CONTEXT_TOKENS = 1024
LATENT_TOKENS = 4096
N_TP = 4


def draw_w_scale(key, part):
    first, second = jax.random.split(jax.random.fold_in(key, 11))
    spread = 2.0 / math.sqrt(MODEL_WIDTH)
    values = jnp.clip(jax.random.normal(first, (MODEL_WIDTH, MODEL_WIDTH), jnp.float32) * spread, -3.0 * spread, 3.0 * spread)
    return values.astype(jnp.bfloat16)


def level_of(stream_key, dims, cuts, least, largest):
    loudness, own = 1.0, jax.random.fold_in(stream_key, 6)
    for dim, shards_of in cuts:
        draws = jnp.exp(jax.random.uniform(jax.random.fold_in(own, dim), (shards_of,), jnp.float32, least / len(cuts), largest / len(cuts)))
        loudness = loudness * jnp.repeat(draws, dims[dim] // shards_of).reshape([-1 if axis == dim else 1 for axis in range(len(dims))])
    return loudness


def normal_values(stream_key, dims, scale, most, shards=(), kind=jnp.bfloat16):
    level = level_of(stream_key, dims, shards, -0.22, 0.18) if shards else 1.0
    values = jax.random.normal(stream_key, dims, jnp.float32) * scale * level
    return jnp.minimum(jnp.maximum(values, -most), most).astype(kind)


def setup_inputs(seed: int = 0) -> dict:
    splits = jax.random.split(jax.random.key(seed), 13)
    return {
        "latent": normal_values(splits[0], (LATENT_TOKENS, MODEL_WIDTH), 0.5, 3.0, ((0, 32),)),
        "context": normal_values(splits[1], (CONTEXT_TOKENS, MODEL_WIDTH), 1.0, 6.0, ((0, 8),)),
        "cond": normal_values(splits[2], (MODEL_WIDTH,), 1.0, 6.0, (), jnp.float32),
        "ctx_cond": normal_values(splits[3], (MODEL_WIDTH,), 1.0, 6.0, (), jnp.float32),
        "w_shift": normal_values(splits[4], (MODEL_WIDTH, MODEL_WIDTH), (MODEL_WIDTH // 4) ** -0.5, 0.1875, ((0, 8), (1, 4))),
        "w_scale": draw_w_scale(jax.random.fold_in(splits[12], 71), 0),
        "w_gate": normal_values(splits[6], (MODEL_WIDTH, MODEL_WIDTH), (MODEL_WIDTH // 4) ** -0.5, 0.1875, ((0, 8), (1, 4))),
        "w_query": normal_values(splits[7], (MODEL_WIDTH, QUERY_HEADS * HEAD_SIZE), MODEL_WIDTH ** -0.5, 0.09375, ((1, 4),)),
        "key_weight": normal_values(splits[8], (MODEL_WIDTH, KEY_VALUE_HEADS * HEAD_SIZE), MODEL_WIDTH ** -0.5, 0.09375, ((1, 4),)),
        "value_weight": normal_values(splits[9], (MODEL_WIDTH, KEY_VALUE_HEADS * HEAD_SIZE), MODEL_WIDTH ** -0.5, 0.09375, ((1, 4),)),
        "w_out": normal_values(splits[10], (QUERY_HEADS * HEAD_SIZE, MODEL_WIDTH), (QUERY_HEADS * HEAD_SIZE) ** -0.5, 0.125, ((0, 4),)),
        "sink": jnp.clip(jax.random.uniform(splits[11], (QUERY_HEADS,), jnp.float32, 4.0, 8.0), 4.0, 8.0),
    }


EPS = 1e-05
THETA = 10000.0
MASKED = -1e+30

def layer_norm(rows):
    values = rows.astype(jnp.float32)
    mean = lax.optimization_barrier(jnp.mean(values, axis=-1, keepdims=True))
    var = lax.optimization_barrier(jnp.mean(jnp.square(values - mean), axis=-1, keepdims=True))
    return (values - mean) * lax.rsqrt(var + EPS)

def rotate_half(values, token_position, width):
    half = width // 2
    inverse = THETA ** (-jnp.arange(half, dtype=jnp.float32) * 2.0 / width)
    angle = token_position.astype(jnp.float32)[:, None] * inverse[None, :]
    cosine = jnp.cos(angle)[:, None, :]
    sine = jnp.sin(angle)[:, None, :]
    first = values[..., :half]
    second = values[..., half:]
    return jnp.concatenate([first * cosine - second * sine, second * cosine + first * sine], axis=-1)

def axial_rotation(heads, token_position, grid):
    width = heads.shape[-1] // 2
    values = heads.astype(jnp.float32)
    turned = jnp.concatenate([rotate_half(values[..., :width], token_position // grid, width), rotate_half(values[..., width:], token_position % grid, width)], axis=-1)
    return turned.astype(jnp.bfloat16)

def sink_weights(scores, sink_column):
    top = jnp.maximum(lax.optimization_barrier(jnp.max(scores, axis=-1, keepdims=True)), sink_column)
    expo = jnp.exp(scores - top)
    return (expo / (lax.optimization_barrier(jnp.sum(expo, axis=-1, keepdims=True)) + jnp.exp(sink_column - top))).astype(jnp.bfloat16)

def reference(latent, context, cond, ctx_cond, w_shift, w_scale, w_gate, w_query, key_weight, value_weight, w_out, sink):
    act = jax.nn.silu(jnp.stack([cond, ctx_cond])).astype(jnp.bfloat16)
    shift = jnp.dot(act, w_shift, preferred_element_type=jnp.float32)
    scale = jnp.dot(act, w_scale, preferred_element_type=jnp.float32)
    gate = jnp.dot(act[0:1], w_gate, preferred_element_type=jnp.float32)[0]
    latent_mod = (layer_norm(latent) * (1.0 + scale[0]) + shift[0]).astype(jnp.bfloat16)
    ctx_mod = (layer_norm(context) * (1.0 + scale[1]) + shift[1]).astype(jnp.bfloat16)
    query_group = QUERY_HEADS // KEY_VALUE_HEADS
    query = jnp.dot(latent_mod, w_query, preferred_element_type=jnp.float32).astype(jnp.bfloat16)
    key = jnp.dot(latent_mod, key_weight, preferred_element_type=jnp.float32).astype(jnp.bfloat16)
    value_rows = jnp.dot(latent_mod, value_weight, preferred_element_type=jnp.float32).astype(jnp.bfloat16)
    context_key_rows = jnp.dot(ctx_mod, key_weight, preferred_element_type=jnp.float32).astype(jnp.bfloat16)
    context_value_rows = jnp.dot(ctx_mod, value_weight, preferred_element_type=jnp.float32).astype(jnp.bfloat16)
    token_position = jnp.arange(LATENT_TOKENS, dtype=jnp.int32)
    rotated_query = axial_rotation(query.reshape(LATENT_TOKENS, QUERY_HEADS, HEAD_SIZE), token_position, GRID_WIDTH)
    rotated_key = axial_rotation(key.reshape(LATENT_TOKENS, KEY_VALUE_HEADS, HEAD_SIZE), token_position, GRID_WIDTH)
    padded_key = jnp.pad(rotated_key, ((WINDOW_SIDE, WINDOW_SIDE), (0, 0), (0, 0)))
    value_padded_rows = jnp.pad(value_rows.reshape(LATENT_TOKENS, KEY_VALUE_HEADS, HEAD_SIZE), ((WINDOW_SIDE, WINDOW_SIDE), (0, 0), (0, 0)))
    context_key_wide = context_key_rows.reshape(CONTEXT_TOKENS, KEY_VALUE_HEADS, HEAD_SIZE).astype(jnp.float32)
    context_value_wide = context_value_rows.reshape(CONTEXT_TOKENS, KEY_VALUE_HEADS, HEAD_SIZE).astype(jnp.float32)
    sink_column = sink.reshape(KEY_VALUE_HEADS, query_group)[:, :, None, None]
    factor = HEAD_SIZE ** (-0.5)
    block_list = LATENT_TOKENS // WINDOW_SIDE
    query_block_list = rotated_query.reshape(block_list, WINDOW_SIDE, KEY_VALUE_HEADS, query_group, HEAD_SIZE)

    def one_block(item):
        qblk, index = item
        start = (index * WINDOW_SIDE).astype(jnp.int32)
        kblk = lax.dynamic_slice_in_dim(padded_key, start, 3 * WINDOW_SIDE, 0).astype(jnp.float32)
        vblk = lax.dynamic_slice_in_dim(value_padded_rows, start, 3 * WINDOW_SIDE, 0).astype(jnp.float32)
        q32 = qblk.astype(jnp.float32)
        band_scores = jnp.einsum('qhgd,khd->hgqk', q32, kblk) * factor
        qpos = start + jnp.arange(WINDOW_SIDE, dtype=jnp.int32)
        kpos = start - WINDOW_SIDE + jnp.arange(3 * WINDOW_SIDE, dtype=jnp.int32)
        valid = (jnp.abs(kpos[None, :] - qpos[:, None]) <= WINDOW_SIDE) & (kpos[None, :] >= 0) & (kpos[None, :] < LATENT_TOKENS)
        band_scores = jnp.where(valid[None, None], band_scores, MASKED)
        ctx_scores = jnp.einsum('qhgd,khd->hgqk', q32, context_key_wide) * factor
        weights = sink_weights(jnp.concatenate([band_scores, ctx_scores], axis=-1), sink_column).astype(jnp.float32)
        out = jnp.einsum('hgqk,khd->qhgd', weights[..., :3 * WINDOW_SIDE], vblk) + jnp.einsum('hgqk,khd->qhgd', weights[..., 3 * WINDOW_SIDE:], context_value_wide)
        return out.astype(jnp.bfloat16).reshape(WINDOW_SIDE, QUERY_HEADS * HEAD_SIZE)
    attended = lax.map(one_block, (query_block_list, jnp.arange(block_list, dtype=jnp.int32))).reshape(LATENT_TOKENS, QUERY_HEADS * HEAD_SIZE)
    columns = QUERY_HEADS * HEAD_SIZE // N_TP
    projected = jnp.zeros((LATENT_TOKENS, MODEL_WIDTH), jnp.float32)
    for group_index in range(N_TP):
        lower = group_index * columns
        partial_product = jnp.dot(attended[:, lower:lower + columns], w_out[lower:lower + columns], preferred_element_type=jnp.float32).astype(jnp.bfloat16)
        projected = projected + partial_product.astype(jnp.float32)
    return (latent.astype(jnp.float32) + gate[None, :] * projected).astype(jnp.bfloat16)
```

```python
import functools
import math

import jax
import jax.numpy as jnp
from jax import lax
from jax.experimental import pallas as pl
from jax.experimental.pallas import tpu as pltpu
from jax.sharding import PartitionSpec as P

HEAD = 128
SIDE = 128
GRID_WIDTH = 64
EPS = 1e-05
THETA = 10000.0
MASKED = -1e30
LOG2E = math.log2(math.e)
MESH = pl.DeviceIdType.MESH
F32 = jnp.float32
BF16 = jnp.bfloat16
CUTS = 2
PIECES = 4
CORES = 2


def body(
    nsp, ntp,
    lat, ctx, cond, ctx_cond, w_shift, w_scale, w_gate, w_q, w_k, w_v, w_o, sink, cos_t, sin_t,
    out,
    wmod, wq, wk, wv, wo, latb, ctxb, mb, part, mgath, tot, mod, ctxkv, q_s, kv, att,
    stage, prcv, comb, xrcv,
    load_sem, msend, mrecv, tsend, trecv, lsend, lrecv, fsend, frecv, psend, precv,
    csend, crecv, hsend, hrecv, dsend, drecv, xsend, xrecv,
):
    nx = ntp // CORES
    sp = lax.axis_index("sp")
    tp = lax.axis_index("tp")
    x = lax.div(tp, CORES)
    c = lax.rem(tp, CORES)
    oc = 1 - c
    rows, width = lat.shape
    crows = ctx.shape[0]
    cut = rows // CUTS
    tokens = rows * ntp
    mcols = w_shift.shape[1]
    qc = w_q.shape[1]
    kc = w_k.shape[1]
    kv_heads = kc // HEAD
    group = qc // kc

    def at_tp(t):
        return (sp, t)

    def at_sp(s):
        return (s, tp)

    partner = at_tp(x * CORES + oc)

    def remote(src, dst, ss, rs, dev):
        return pltpu.make_async_remote_copy(
            src_ref=src, dst_ref=dst, send_sem=ss, recv_sem=rs, device_id=dev, device_id_type=MESH
        )

    loads = [
        pltpu.make_async_copy(s, d, load_sem.at[i])
        for i, (s, d) in enumerate(
            [
                (w_shift, wmod.at[0]), (w_scale, wmod.at[1]), (w_gate, wmod.at[2]),
                (ctx, ctxb), (w_k, wk), (w_v, wv), (w_q, wq),
                (lat, latb.at[tp]), (w_o, wo),
            ]
        )
    ]
    for load in loads:
        load.start()

    barrier = pltpu.get_barrier_semaphore()
    for d in range(1, nsp):
        pl.semaphore_signal(barrier, inc=1, device_id=at_sp(lax.rem(sp + d, nsp)), device_id_type=MESH)
    for d in range(1, ntp):
        pl.semaphore_signal(barrier, inc=1, device_id=at_tp(lax.rem(tp + d, ntp)), device_id_type=MESH)
    pl.semaphore_wait(barrier, nsp + ntp - 2)

    def lat_copy(d, j):
        dst = lax.rem(x + d, nx) * CORES + c
        return remote(
            lat.at[pl.ds(j * cut, cut)], latb.at[tp, pl.ds(j * cut, cut)],
            lsend.at[d - 1, j], lrecv.at[d - 1, j], at_tp(dst),
        )

    def from_x(d):
        return lax.rem(x - d + nx, nx)

    def fwd_copy(d, j):
        slot = latb.at[from_x(d) * CORES + c, pl.ds(j * cut, cut)]
        return remote(slot, slot, fsend.at[d - 1, j], frecv.at[d - 1, j], partner)

    for d in range(1, nx):
        lat_copy(d, 0).start()
    own = remote(lat, latb.at[tp], psend, precv, partner)
    own.start()

    a0 = jax.nn.silu(cond[pl.ds(sp, 1), :]).astype(BF16).astype(F32)
    a1 = jax.nn.silu(ctx_cond[pl.ds(sp, 1), :]).astype(BF16).astype(F32)
    line = lax.broadcasted_iota(jnp.int32, (8, a0.shape[1]), 0)
    z = jnp.zeros((8, a0.shape[1]), F32)
    a0 = jnp.broadcast_to(a0, z.shape)
    a1 = jnp.broadcast_to(a1, z.shape)
    acc = None
    for i, (r0, r1) in enumerate(((0, 1), (2, 3), (4, -1))):
        act = jnp.where(line == r0, a0, jnp.where(line == r1, a1, z)).astype(BF16)
        loads[i].wait()
        piece = jnp.dot(act, wmod[i], preferred_element_type=F32)
        acc = piece if acc is None else acc + piece
    part[...] = acc
    mcopies = [
        remote(part, mgath.at[d - 1], msend.at[d - 1], mrecv.at[d - 1], at_sp(lax.rem(sp + d, nsp)))
        for d in range(1, nsp)
    ]
    for cp in mcopies:
        cp.start()
    for i in range(3, 8):
        loads[i].wait()
    acc = part[...]
    for d in range(1, nsp):
        mcopies[d - 1].wait_recv()
        acc = acc + mgath[d - 1]
    tot[...] = acc
    mine = pl.ds(pl.multiple_of(tp * mcols, mcols), mcols)
    tcopies = [
        remote(tot, mod.at[:, mine], tsend.at[d - 1], trecv.at[d - 1], at_tp(lax.rem(tp + d, ntp)))
        for d in range(1, ntp)
    ]
    for cp in tcopies:
        cp.start()
    for d in range(1, nx):
        for j in range(1, CUTS):
            lat_copy(d, j).start()
    mod[:, mine] = acc
    for cp in tcopies:
        cp.wait_recv()

    def normed(src, row0, dst, dst0, count, r_shift, r_scale):
        step = 16

        @pl.loop(0, count // step)
        def _(i):
            v = src[pl.ds(row0 + i * step, step), :].astype(F32)
            mean = jnp.mean(v, axis=-1, keepdims=True)
            v = v - mean
            var = jnp.mean(v * v, axis=-1, keepdims=True)
            v = v * lax.rsqrt(var + EPS)
            v = v * (1.0 + mod[r_scale : r_scale + 1, :]) + mod[r_shift : r_shift + 1, :]
            dst[pl.ds(dst0 + i * step, step), :] = v.astype(BF16)

    normed(ctxb, 0, mb, 0, crows, 1, 3)
    crow = pl.ds(pl.multiple_of(sp * crows, crows), crows)
    cm = mb[0:crows, :]
    ctxkv[crow, 0:kc] = jnp.dot(cm, wk[...], preferred_element_type=F32).astype(BF16)
    ctxkv[crow, kc : 2 * kc] = jnp.dot(cm, wv[...], preferred_element_type=F32).astype(BF16)
    ccopies = [
        remote(ctxkv.at[crow], ctxkv.at[crow], csend.at[d - 1], crecv.at[d - 1], at_sp(lax.rem(sp + d, nsp)))
        for d in range(1, nsp)
    ]
    for cp in ccopies:
        cp.start()

    for d in range(1, nx):
        lat_copy(d, 0).wait_recv()
        fwd_copy(d, 0).start()

    lane = lax.broadcasted_iota(jnp.int32, (1, HEAD), 1)
    low = lax.rem(lane, HEAD // 2) < HEAD // 4

    def turn(v, row0, count, factor):
        v = v.astype(BF16).astype(F32)
        swapped = jnp.where(low, pltpu.roll(v, HEAD - HEAD // 4, 1), pltpu.roll(v, HEAD // 4, 1))
        r = v * cos_t[pl.ds(row0, count), :] + swapped * sin_t[pl.ds(row0, count), :]
        return (r * factor).astype(BF16)

    def project(segments):
        total = sum(n for _, n in segments)
        qf = HEAD ** (-0.5) * LOG2E
        for w, cols, kind in ((wq, qc, 0), (wk, kc, 1), (wv, kc, 2)):
            tile = min(256, cols)
            for n0 in range(0, cols, tile):
                r = jnp.dot(mb[0:total, :], w[:, n0 : n0 + tile], preferred_element_type=F32)
                off = 0
                for row0, n in segments:
                    for h in range(0, tile, HEAD):
                        v = r[off : off + n, h : h + HEAD]
                        if kind == 0:
                            q_s[pl.ds(row0, n), n0 + h : n0 + h + HEAD] = turn(v, row0, n, qf)
                        elif kind == 1:
                            kv[pl.ds(row0 + SIDE, n), n0 + h : n0 + h + HEAD] = turn(v, row0, n, 1.0)
                        else:
                            kv[pl.ds(row0 + SIDE, n), kc + n0 + h : kc + n0 + h + HEAD] = v.astype(BF16)
                    off += n

    lat2 = latb.reshape(ntp * rows, width)
    own.wait_recv()
    base = pl.multiple_of(x * CORES * rows, CORES * rows)
    normed(lat2, base, mb, 0, CORES * rows, 0, 2)
    project([(base, CORES * rows)])

    left = at_sp(lax.rem(sp + nsp - 1, nsp))
    right = at_sp(lax.rem(sp + 1, nsp))
    to_left = remote(kv.at[pl.ds(SIDE, SIDE)], kv.at[pl.ds(SIDE + tokens, SIDE)], hsend.at[0], hrecv.at[0], left)
    to_right = remote(kv.at[pl.ds(tokens, SIDE)], kv.at[pl.ds(0, SIDE)], hsend.at[1], hrecv.at[1], right)

    @pl.when(x == 0)
    def _():
        to_left.start()

    @pl.when(x == nx - 1)
    def _():
        to_right.start()

    for d in range(1, nx):
        for j in range(CUTS):
            if j > 0:
                lat_copy(d, j).wait_recv()
                fwd_copy(d, j).start()
            r_a = pl.multiple_of((from_x(d) * CORES + c) * rows + j * cut, cut)
            r_b = pl.multiple_of((from_x(d) * CORES + oc) * rows + j * cut, cut)
            normed(lat2, r_a, mb, 0, cut, 0, 2)
            fwd_copy(d, j).wait_recv()
            normed(lat2, r_b, mb, cut, cut, 0, 2)
            project([(r_a, cut), (r_b, cut)])

    @pl.when(x != 0)
    def _():
        to_left.start()

    @pl.when(x != nx - 1)
    def _():
        to_right.start()

    for cp in ccopies:
        cp.wait_recv()
    loads[8].wait()

    band = rows + 2 * SIDE
    key_i = lax.broadcasted_iota(jnp.int32, (rows, band), 1)
    gap = key_i - lax.broadcasted_iota(jnp.int32, (rows, band), 0)
    near = (gap >= 0) & (gap <= 2 * SIDE)

    def attend(t):
        r0 = pl.multiple_of(t * rows, rows)
        kpos = key_i + (sp * tokens + r0 - SIDE)
        valid = near & (kpos >= 0) & (kpos < tokens * nsp)
        bias = jnp.where(valid, 0.0, MASKED)
        bias = jnp.concatenate([bias] * group, axis=0)
        for h in range(kv_heads):
            heads = [h * group + i for i in range(group)]
            q = jnp.concatenate([q_s[pl.ds(r0, rows), j * HEAD : (j + 1) * HEAD] for j in heads], axis=0)
            kb = kv[pl.ds(r0, band), h * HEAD : (h + 1) * HEAD]
            vb = kv[pl.ds(r0, band), kc + h * HEAD : kc + (h + 1) * HEAD]
            kx = ctxkv[:, h * HEAD : (h + 1) * HEAD]
            vx = ctxkv[:, kc + h * HEAD : kc + (h + 1) * HEAD]
            dims = (((1,), (1,)), ((), ()))
            sb = lax.dot_general(q, kb, dims, preferred_element_type=F32) + bias
            sx = lax.dot_general(q, kx, dims, preferred_element_type=F32)
            snk = jnp.concatenate(
                [jnp.broadcast_to(sink[pl.ds(tp * (qc // HEAD) + j, 1), 0:1], (rows, 1)) for j in heads], axis=0
            ) * LOG2E
            top = jnp.maximum(
                jnp.maximum(jnp.max(sb, axis=-1, keepdims=True), jnp.max(sx, axis=-1, keepdims=True)), snk
            )
            eb = jnp.exp2(sb - top)
            ex = jnp.exp2(sx - top)
            den = jnp.sum(eb, axis=-1, keepdims=True) + jnp.sum(ex, axis=-1, keepdims=True) + jnp.exp2(snk - top)
            o = jnp.dot(eb.astype(BF16), vb, preferred_element_type=F32) + jnp.dot(
                ex.astype(BF16), vx, preferred_element_type=F32
            )
            o = (o / den).astype(BF16)
            for i, j in enumerate(heads):
                att[:, j * HEAD : (j + 1) * HEAD] = o[i * rows : (i + 1) * rows]

    piece_rows = rows // PIECES
    ntile = min(512, width)

    def x_copy(g, p, xo):
        return remote(
            comb.at[g, pl.ds(p * piece_rows, piece_rows)], xrcv.at[g, pl.ds(p * piece_rows, piece_rows)],
            xsend.at[g, p], xrecv.at[g, p], at_tp(xo * CORES + c),
        )

    def d_copy(g):
        return remote(stage.at[g, 0], prcv.at[g], dsend.at[g], drecv.at[g], partner)

    for g in range(nx):
        xo = lax.rem(x + 1 + g, nx)
        if g == 0:
            @pl.when(x != 0)
            def _():
                to_right.wait_recv()

            @pl.when(x != nx - 1)
            def _():
                to_left.wait_recv()
        if g == nx - 1:
            @pl.when(x == 0)
            def _():
                to_right.wait_recv()

            @pl.when(x == nx - 1)
            def _():
                to_left.wait_recv()

        @pl.loop(0, 2)
        def _(u):
            attend(xo * CORES + lax.rem(oc + u, 2))

            @pl.loop(0, width // ntile)
            def _(n):
                cs = pl.ds(pl.multiple_of(n * ntile, ntile), ntile)
                stage[g, u, :, cs] = jnp.dot(att[...], wo[:, cs], preferred_element_type=F32).astype(BF16)

            @pl.when(u == 0)
            def _():
                d_copy(g).start()

        d_copy(g).wait_recv()
        if g < nx - 1:
            for p in range(PIECES):
                sl = slice(p * piece_rows, (p + 1) * piece_rows)
                comb[g, sl, :] = (stage[g, 1, sl, :].astype(F32) + prcv[g, sl, :].astype(F32)).astype(BF16)
                x_copy(g, p, xo).start()

    last = nx - 1
    for p in range(PIECES):
        sl = slice(p * piece_rows, (p + 1) * piece_rows)
        total = stage[last, 1, sl, :].astype(F32) + prcv[last, sl, :].astype(F32)
        for g in range(nx - 1):
            x_copy(g, p, lax.rem(x + 1 + g, nx)).wait_recv()
            total = total + xrcv[g, sl, :].astype(F32)
        base_rows = latb[tp, sl, :].astype(F32)
        out[sl, :] = (base_rows + mod[4:5, :] * total).astype(BF16)

    for cp in mcopies + tcopies + ccopies + [own, to_left, to_right]:
        cp.wait_send()
    for d in range(1, nx):
        for j in range(CUTS):
            lat_copy(d, j).wait_send()
            fwd_copy(d, j).wait_send()
    for g in range(nx):
        d_copy(g).wait_send()
        if g < nx - 1:
            for p in range(PIECES):
                x_copy(g, p, lax.rem(x + 1 + g, nx)).wait_send()


def shards(lat, ctx, cond, ctx_cond, w_shift, w_scale, w_gate, w_q, w_k, w_v, w_o, sink):
    nsp = lax.axis_size("sp")
    ntp = lax.axis_size("tp")
    nx = ntp // CORES
    rows, width = lat.shape
    crows = ctx.shape[0]
    tokens = rows * ntp
    qc = w_q.shape[1]
    kc = w_k.shape[1]
    mrows, mcols = w_shift.shape
    half = HEAD // 2
    lane = jnp.arange(HEAD)
    inverse = THETA ** (-(lane % (half // 2)).astype(F32) * 2.0 / half)
    pos = lax.axis_index("sp") * tokens + jnp.arange(tokens, dtype=jnp.int32)[:, None]
    spot = jnp.where(lane[None, :] < half, pos // GRID_WIDTH, pos % GRID_WIDTH).astype(F32)
    angle = spot * inverse[None, :]
    cos_t = jnp.cos(angle)
    sin_t = jnp.sin(angle) * jnp.where(lane % half < half // 2, -1.0, 1.0)[None, :]
    sink_b = jnp.broadcast_to(sink[:, None], (sink.shape[0], 128))

    any_ = pl.BlockSpec(memory_space=pl.ANY)
    vmem = pl.BlockSpec(memory_space=pltpu.VMEM)
    dma = pltpu.SemaphoreType.DMA
    V = pltpu.VMEM
    return pl.pallas_call(
        functools.partial(body, nsp, ntp),
        out_shape=jax.ShapeDtypeStruct((rows, width), BF16),
        in_specs=[any_, any_, vmem, vmem] + [any_] * 7 + [vmem] * 3,
        out_specs=vmem,
        scratch_shapes=[
            V((3, mrows, mcols), BF16), V((width, qc), BF16), V((width, kc), BF16), V((width, kc), BF16),
            V((qc, width), BF16), V((ntp, rows, width), BF16), V((crows, width), BF16),
            V((max(CORES * rows, crows), width), BF16), V((8, mcols), F32), V((nsp - 1, 8, mcols), F32),
            V((8, mcols), F32), V((8, width), F32), V((nsp * crows, 2 * kc), BF16), V((tokens, qc), BF16),
            V((tokens + 2 * SIDE, 2 * kc), BF16), V((rows, qc), BF16),
            V((nx, 2, rows, width), BF16), V((nx, rows, width), BF16),
            V((nx - 1, rows, width), BF16), V((nx - 1, rows, width), BF16),
            dma((9,)), dma((nsp - 1,)), dma((nsp - 1,)), dma((ntp - 1,)), dma((ntp - 1,)),
            dma((nx - 1, CUTS)), dma((nx - 1, CUTS)), dma((nx - 1, CUTS)), dma((nx - 1, CUTS)), dma, dma,
            dma((nsp - 1,)), dma((nsp - 1,)), dma((2,)), dma((2,)), dma((nx,)), dma((nx,)),
            dma((nx - 1, PIECES)), dma((nx - 1, PIECES)),
        ],
        compiler_params=pltpu.CompilerParams(
            collective_id=0, has_side_effects=True, vmem_limit_bytes=60 * 1024 * 1024
        ),
    )(
        lat, ctx, cond.reshape(nsp, mrows), ctx_cond.reshape(nsp, mrows),
        w_shift, w_scale, w_gate, w_q, w_k, w_v, w_o, sink_b, cos_t, sin_t,
    )


def solution(mesh):
    in_specs = (
        P(("sp", "tp"), None), P("sp", None), P(), P(), P("sp", "tp"), P("sp", "tp"), P("sp", "tp"),
        P(None, "tp"), P(None, "tp"), P(None, "tp"), P("tp", None), P(),
    )
    return jax.shard_map(
        shards, mesh=mesh, in_specs=in_specs, out_specs=P(("sp", "tp"), None), check_vma=False
    )
```

```python
import functools
import math

import jax
import jax.numpy as jnp
from jax import lax
from jax.experimental import pallas as pl
from jax.experimental.pallas import tpu as pltpu
from jax.sharding import PartitionSpec as P

HEAD = 128
SIDE = 128
GRID_WIDTH = 64
EPS = 1e-05
THETA = 10000.0
MASKED = -1e30
LOG2E = math.log2(math.e)
MESH = pl.DeviceIdType.MESH
F32 = jnp.float32
BF16 = jnp.bfloat16
CUTS = 2
TILES = 4
CORES = 2


def body(
    nsp, ntp,
    lat, ctx, cond, ctx_cond, w_shift, w_scale, w_gate, w_q, w_k, w_v, w_o, sink,
    out,
    cos_t, sin_t, st_mean, st_rstd, tslots,
    wmod, wq, wk, wv, wo, latb, ctxb, mb, part, mgath, mod, ctxkv, q_s, kv, att,
    stage, prcv, comb, xrcv,
    load_sem, msend, mrecv, tsend, trecv, lsend, lrecv, fsend, frecv, psend, precv,
    csend, crecv, hsend, hrecv, dsend, drecv, xsend, xrecv,
):
    nx = ntp // CORES
    sp = lax.axis_index("sp")
    tp = lax.axis_index("tp")
    x = lax.div(tp, CORES)
    c = lax.rem(tp, CORES)
    oc = 1 - c
    rows, width = lat.shape
    crows = ctx.shape[0]
    cut = rows // CUTS
    tokens = rows * ntp
    mcols = w_shift.shape[1]
    qc = w_q.shape[1]
    kc = w_k.shape[1]
    kv_heads = kc // HEAD
    group = qc // kc

    def at_tp(t):
        return (sp, t)

    def at_sp(s):
        return (s, tp)

    partner = at_tp(x * CORES + oc)

    def remote(src, dst, ss, rs, dev):
        return pltpu.make_async_remote_copy(
            src_ref=src, dst_ref=dst, send_sem=ss, recv_sem=rs, device_id=dev, device_id_type=MESH
        )

    loads = [
        pltpu.make_async_copy(s, d, load_sem.at[i])
        for i, (s, d) in enumerate(
            [
                (w_shift, wmod.at[0]), (w_scale, wmod.at[1]), (w_gate, wmod.at[2]),
                (ctx, ctxb), (w_k, wk), (w_v, wv), (w_q, wq),
                (lat, latb.at[tp]), (w_o, wo),
            ]
        )
    ]
    for load in loads[:3]:
        load.start()

    barrier = pltpu.get_barrier_semaphore()
    for d in range(1, nsp):
        pl.semaphore_signal(barrier, inc=1, device_id=at_sp(lax.rem(sp + d, nsp)), device_id_type=MESH)
    for d in range(1, ntp):
        pl.semaphore_signal(barrier, inc=1, device_id=at_tp(lax.rem(tp + d, ntp)), device_id_type=MESH)
    pl.semaphore_wait(barrier, nsp + ntp - 2)

    def lat_copy(d, j):
        dst = lax.rem(x + d, nx) * CORES + c
        return remote(
            lat.at[pl.ds(j * cut, cut)], latb.at[tp, pl.ds(j * cut, cut)],
            lsend.at[d - 1, j], lrecv.at[d - 1, j], at_tp(dst),
        )

    def from_x(d):
        return lax.rem(x - d + nx, nx)

    def fwd_copy(d, j):
        slot = latb.at[from_x(d) * CORES + c, pl.ds(j * cut, cut)]
        return remote(slot, slot, fsend.at[d - 1, j], frecv.at[d - 1, j], partner)

    for d in range(1, nx):
        lat_copy(d, 0).start()
    own = remote(lat, latb.at[tp], psend, precv, partner)
    own.start()

    mrows = w_shift.shape[0]
    arow = pl.ds(pl.multiple_of(sp * mrows, mrows), mrows)
    a0 = jax.nn.silu(cond[arow].reshape(1, mrows)).astype(BF16).astype(F32)
    a1 = jax.nn.silu(ctx_cond[arow].reshape(1, mrows)).astype(BF16).astype(F32)
    line = lax.broadcasted_iota(jnp.int32, (8, a0.shape[1]), 0)
    line8 = lax.broadcasted_iota(jnp.int32, (8, mcols // 2), 0)
    z = jnp.zeros((8, a0.shape[1]), F32)
    a0 = jnp.broadcast_to(a0, z.shape)
    a1 = jnp.broadcast_to(a1, z.shape)
    acc = None
    for i, (r0, r1) in enumerate(((0, 1), (2, 3), (4, -1))):
        act = jnp.where(line == r0, a0, jnp.where(line == r1, a1, z)).astype(BF16)
        loads[i].wait()
        piece = jnp.dot(act, wmod[i], preferred_element_type=F32)
        acc = piece if acc is None else acc + piece
    hc = mcols // 2
    part[...] = jnp.concatenate([acc[:, :hc], acc[:, hc:]], axis=0).astype(BF16)
    mcopies = [
        remote(part, mgath.at[d - 1], msend.at[d - 1], mrecv.at[d - 1], at_sp(lax.rem(sp + d, nsp)))
        for d in range(1, nsp)
    ]
    for cp in mcopies:
        cp.start()
    for i in (3, 7, 4, 5, 6, 8):
        loads[i].start()

    def turn_tables():
        half = HEAD // 2
        lane_i = lax.broadcasted_iota(jnp.int32, (tokens, HEAD), 1)
        inner = lax.rem(lane_i, half // 2).astype(F32)
        inverse = jnp.exp(inner * (-2.0 / half * math.log(THETA)))
        pos = (lax.broadcasted_iota(jnp.int32, (tokens, HEAD), 0) + sp * tokens).astype(F32)
        grid_row = jnp.floor(pos * (1.0 / GRID_WIDTH))
        angle = jnp.where(lane_i < half, grid_row, pos - grid_row * GRID_WIDTH) * inverse
        cos_t[...] = jnp.cos(angle)
        sin_t[...] = jnp.where(lax.rem(lane_i, half) < half // 2, -1.0, 1.0) * jnp.sin(angle)

    step = 16

    def measure_rows(src, row0, st0, count):
        @pl.loop(0, count // step)
        def _(i):
            v = src[pl.ds(row0 + i * step, step), :].astype(F32)
            mean = jnp.mean(v, axis=-1, keepdims=True)
            v = v - mean
            var = jnp.mean(v * v, axis=-1, keepdims=True)
            st_mean[pl.ds(st0 + i * step, step), :] = jnp.broadcast_to(mean, (step, HEAD))
            st_rstd[pl.ds(st0 + i * step, step), :] = jnp.broadcast_to(lax.rsqrt(var + EPS), (step, HEAD))

    def shift_rows(src, row0, st0, dst, dst0, count, r_shift, r_scale):
        @pl.loop(0, count // step)
        def _(i):
            v = src[pl.ds(row0 + i * step, step), :].astype(F32)
            srow = pl.ds(st0 + i * step, step)
            v = (v - st_mean[srow, 0:1]) * st_rstd[srow, 0:1]
            v = v * mod[r_scale : r_scale + 1, :] + mod[r_shift : r_shift + 1, :]
            dst[pl.ds(dst0 + i * step, step), :] = v.astype(BF16)

    lat2 = latb.reshape(ntp * rows, width)
    base = pl.multiple_of(x * CORES * rows, CORES * rows)
    loads[3].wait()
    measure_rows(ctxb, 0, 0, crows)
    acc = part[...].astype(F32)
    for d in range(1, nsp):
        mcopies[d - 1].wait_recv()
        acc = acc + mgath[d - 1].astype(F32)
    tslots[tp] = acc.astype(BF16)
    tcopies = [
        remote(tslots.at[tp], tslots.at[tp], tsend.at[d - 1], trecv.at[d - 1], at_tp(lax.rem(tp + d, ntp)))
        for d in range(1, ntp)
    ]
    for cp in tcopies:
        cp.start()
    for d in range(1, nx):
        for j in range(1, CUTS):
            lat_copy(d, j).start()
    turn_tables()
    for cp in tcopies:
        cp.wait_recv()
    for t in range(ntp):
        v = tslots[t].astype(F32)
        bump = jnp.where((line8 == 2) | (line8 == 3), 1.0, 0.0)
        mod[:, t * mcols : t * mcols + hc] = v[0:8] + bump
        mod[:, t * mcols + hc : (t + 1) * mcols] = v[8:16] + bump
    loads[4].wait()
    loads[5].wait()

    shift_rows(ctxb, 0, 0, mb, 0, crows, 1, 3)
    crow = pl.ds(pl.multiple_of(sp * crows, crows), crows)
    cm = mb[0:crows, :]
    ctxkv[crow, 0:kc] = jnp.dot(cm, wk[...], preferred_element_type=F32).astype(BF16)
    ctxkv[crow, kc : 2 * kc] = jnp.dot(cm, wv[...], preferred_element_type=F32).astype(BF16)
    ccopies = [
        remote(ctxkv.at[crow], ctxkv.at[crow], csend.at[d - 1], crecv.at[d - 1], at_sp(lax.rem(sp + d, nsp)))
        for d in range(1, nsp)
    ]
    for cp in ccopies:
        cp.start()

    for d in range(1, nx):
        lat_copy(d, 0).wait_recv()
        fwd_copy(d, 0).start()

    lane = lax.broadcasted_iota(jnp.int32, (1, HEAD), 1)
    low = lax.rem(lane, HEAD // 2) < HEAD // 4

    def turn(v, row0, count, factor):
        v = v.astype(BF16).astype(F32)
        swapped = jnp.where(low, pltpu.roll(v, HEAD - HEAD // 4, 1), pltpu.roll(v, HEAD // 4, 1))
        r = v * cos_t[pl.ds(row0, count), :] + swapped * sin_t[pl.ds(row0, count), :]
        return (r * factor).astype(BF16)

    def project(segments):
        total = sum(n for _, n in segments)
        qf = HEAD ** (-0.5) * LOG2E
        for w, cols, kind in ((wq, qc, 0), (wk, kc, 1), (wv, kc, 2)):
            tile = min(256, cols)
            for n0 in range(0, cols, tile):
                r = jnp.dot(mb[0:total, :], w[:, n0 : n0 + tile], preferred_element_type=F32)
                off = 0
                for row0, n in segments:
                    for h in range(0, tile, HEAD):
                        v = r[off : off + n, h : h + HEAD]
                        if kind == 0:
                            q_s[pl.ds(row0, n), n0 + h : n0 + h + HEAD] = turn(v, row0, n, qf)
                        elif kind == 1:
                            kv[pl.ds(row0 + SIDE, n), n0 + h : n0 + h + HEAD] = turn(v, row0, n, 1.0)
                        else:
                            kv[pl.ds(row0 + SIDE, n), kc + n0 + h : kc + n0 + h + HEAD] = v.astype(BF16)
                    off += n

    loads[6].wait()
    loads[7].wait()
    own.wait_recv()
    measure_rows(lat2, base, 0, CORES * rows)
    shift_rows(lat2, base, 0, mb, 0, CORES * rows, 0, 2)
    project([(base, CORES * rows)])

    left = at_sp(lax.rem(sp + nsp - 1, nsp))
    right = at_sp(lax.rem(sp + 1, nsp))
    to_left = remote(kv.at[pl.ds(SIDE, SIDE)], kv.at[pl.ds(SIDE + tokens, SIDE)], hsend.at[0], hrecv.at[0], left)
    to_right = remote(kv.at[pl.ds(tokens, SIDE)], kv.at[pl.ds(0, SIDE)], hsend.at[1], hrecv.at[1], right)

    @pl.when(x == 0)
    def _():
        to_left.start()

    @pl.when(x == nx - 1)
    def _():
        to_right.start()

    for d in range(1, nx):
        for j in range(CUTS):
            if j > 0:
                lat_copy(d, j).wait_recv()
                fwd_copy(d, j).start()
            r_a = pl.multiple_of((from_x(d) * CORES + c) * rows + j * cut, cut)
            r_b = pl.multiple_of((from_x(d) * CORES + oc) * rows + j * cut, cut)
            measure_rows(lat2, r_a, 0, cut)
            shift_rows(lat2, r_a, 0, mb, 0, cut, 0, 2)
            fwd_copy(d, j).wait_recv()
            measure_rows(lat2, r_b, cut, cut)
            shift_rows(lat2, r_b, cut, mb, cut, cut, 0, 2)
            project([(r_a, cut), (r_b, cut)])

    @pl.when(x != 0)
    def _():
        to_left.start()

    @pl.when(x != nx - 1)
    def _():
        to_right.start()

    for cp in ccopies:
        cp.wait_recv()
    loads[8].wait()

    band = rows + 2 * SIDE
    key_i = lax.broadcasted_iota(jnp.int32, (rows, band), 1)
    gap = key_i - lax.broadcasted_iota(jnp.int32, (rows, band), 0)
    near = (gap >= 0) & (gap <= 2 * SIDE)

    def attend(t, u):
        r0 = pl.multiple_of(t * rows, rows)
        kpos = key_i + (sp * tokens + r0 - SIDE)
        valid = near & (kpos >= 0) & (kpos < tokens * nsp)
        bias = jnp.where(valid, 0.0, MASKED)
        bias = jnp.concatenate([bias] * group, axis=0)
        for h in range(kv_heads):
            heads = [h * group + i for i in range(group)]
            q = jnp.concatenate([q_s[pl.ds(r0, rows), j * HEAD : (j + 1) * HEAD] for j in heads], axis=0)
            kb = kv[pl.ds(r0, band), h * HEAD : (h + 1) * HEAD]
            vb = kv[pl.ds(r0, band), kc + h * HEAD : kc + (h + 1) * HEAD]
            kx = ctxkv[:, h * HEAD : (h + 1) * HEAD]
            vx = ctxkv[:, kc + h * HEAD : kc + (h + 1) * HEAD]
            dims = (((1,), (1,)), ((), ()))
            sb = lax.dot_general(q, kb, dims, preferred_element_type=F32) + bias
            sx = lax.dot_general(q, kx, dims, preferred_element_type=F32)
            snk = jnp.concatenate(
                [jnp.full((rows, 1), sink[tp * (qc // HEAD) + j], F32) for j in heads], axis=0
            ) * LOG2E
            top = jnp.maximum(
                jnp.maximum(jnp.max(sb, axis=-1, keepdims=True), jnp.max(sx, axis=-1, keepdims=True)), snk
            )
            eb = jnp.exp2(sb - top)
            ex = jnp.exp2(sx - top)
            den = jnp.sum(eb, axis=-1, keepdims=True) + jnp.sum(ex, axis=-1, keepdims=True) + jnp.exp2(snk - top)
            o = jnp.dot(eb.astype(BF16), vb, preferred_element_type=F32) + jnp.dot(
                ex.astype(BF16), vx, preferred_element_type=F32
            )
            o = (o / den).astype(BF16)
            for i, j in enumerate(heads):
                att[u, :, j * HEAD : (j + 1) * HEAD] = o[i * rows : (i + 1) * rows]

    tile_cols = width // TILES
    ntile = min(512, tile_cols)

    def cols_of(n):
        return slice(n * tile_cols, (n + 1) * tile_cols)

    def x_copy(g, n, xo):
        return remote(
            comb.at[g, n], xrcv.at[g, n], xsend.at[g, n], xrecv.at[g, n], at_tp(xo * CORES + c)
        )

    def d_copy(g, n):
        return remote(stage.at[g, 0, n], prcv.at[g, n], dsend.at[g, n], drecv.at[g, n], partner)

    def combine(g, n, xo):
        d_copy(g, n).wait_recv()
        if g < nx - 1:
            comb[g, n] = (stage[g, 1, n].astype(F32) + prcv[g, n].astype(F32)).astype(BF16)
            x_copy(g, n, xo).start()

    for g in range(nx):
        xo = lax.rem(x + 1 + g, nx)
        if g == 0:
            @pl.when(x != 0)
            def _():
                to_right.wait_recv()

            @pl.when(x != nx - 1)
            def _():
                to_left.wait_recv()
        if g == nx - 1:
            @pl.when(x == 0)
            def _():
                to_right.wait_recv()

            @pl.when(x == nx - 1)
            def _():
                to_left.wait_recv()

        @pl.loop(0, 2)
        def _(u):
            attend(xo * CORES + lax.rem(oc + u, 2), u)

        for n in range(TILES):
            for u in range(2):
                for k in range(0, tile_cols, ntile):
                    stage[g, u, n, :, k : k + ntile] = jnp.dot(
                        att[u], wo[:, n * tile_cols + k : n * tile_cols + k + ntile], preferred_element_type=F32
                    ).astype(BF16)
                if u == 0:
                    d_copy(g, n).start()
            if n > 0:
                combine(g, n - 1, xo)
        combine(g, TILES - 1, xo)

    last = nx - 1
    for n in range(TILES):
        total = stage[last, 1, n].astype(F32) + prcv[last, n].astype(F32)
        for g in range(nx - 1):
            x_copy(g, n, lax.rem(x + 1 + g, nx)).wait_recv()
            total = total + xrcv[g, n].astype(F32)
        out[:, cols_of(n)] = (latb[tp, :, cols_of(n)].astype(F32) + mod[4:5, cols_of(n)] * total).astype(BF16)

    for cp in mcopies + tcopies + ccopies + [own, to_left, to_right]:
        cp.wait_send()
    for d in range(1, nx):
        for j in range(CUTS):
            lat_copy(d, j).wait_send()
            fwd_copy(d, j).wait_send()
    for g in range(nx):
        for n in range(TILES):
            d_copy(g, n).wait_send()
            if g < nx - 1:
                x_copy(g, n, lax.rem(x + 1 + g, nx)).wait_send()


def shards(lat, ctx, cond, ctx_cond, w_shift, w_scale, w_gate, w_q, w_k, w_v, w_o, sink):
    nsp = lax.axis_size("sp")
    ntp = lax.axis_size("tp")
    nx = ntp // CORES
    rows, width = lat.shape
    crows = ctx.shape[0]
    tokens = rows * ntp
    qc = w_q.shape[1]
    kc = w_k.shape[1]
    mrows, mcols = w_shift.shape
    any_ = pl.BlockSpec(memory_space=pl.ANY)
    vmem = pl.BlockSpec(memory_space=pltpu.VMEM)
    dma = pltpu.SemaphoreType.DMA
    V = pltpu.VMEM
    return pl.pallas_call(
        functools.partial(body, nsp, ntp),
        out_shape=jax.ShapeDtypeStruct((rows, width), BF16),
        in_specs=[any_, any_, vmem, vmem] + [any_] * 7 + [pl.BlockSpec(memory_space=pltpu.SMEM)],
        out_specs=vmem,
        scratch_shapes=[
            V((tokens, HEAD), F32), V((tokens, HEAD), F32), V((max(CORES * rows, crows), HEAD), F32),
            V((max(CORES * rows, crows), HEAD), F32), V((ntp, 16, mcols // 2), BF16),
            V((3, mrows, mcols), BF16), V((width, qc), BF16), V((width, kc), BF16), V((width, kc), BF16),
            V((qc, width), BF16), V((ntp, rows, width), BF16), V((crows, width), BF16),
            V((max(CORES * rows, crows), width), BF16), V((16, mcols // 2), BF16), V((nsp - 1, 16, mcols // 2), BF16),
            V((8, width), F32), V((nsp * crows, 2 * kc), BF16), V((tokens, qc), BF16),
            V((tokens + 2 * SIDE, 2 * kc), BF16), V((2, rows, qc), BF16),
            V((nx, 2, TILES, rows, width // TILES), BF16), V((nx, TILES, rows, width // TILES), BF16),
            V((nx - 1, TILES, rows, width // TILES), BF16), V((nx - 1, TILES, rows, width // TILES), BF16),
            dma((9,)), dma((nsp - 1,)), dma((nsp - 1,)), dma((ntp - 1,)), dma((ntp - 1,)),
            dma((nx - 1, CUTS)), dma((nx - 1, CUTS)), dma((nx - 1, CUTS)), dma((nx - 1, CUTS)), dma, dma,
            dma((nsp - 1,)), dma((nsp - 1,)), dma((2,)), dma((2,)), dma((nx, TILES)), dma((nx, TILES)),
            dma((nx - 1, TILES)), dma((nx - 1, TILES)),
        ],
        compiler_params=pltpu.CompilerParams(
            collective_id=0, has_side_effects=True, vmem_limit_bytes=60 * 1024 * 1024
        ),
    )(
        lat, ctx, cond, ctx_cond,
        w_shift, w_scale, w_gate, w_q, w_k, w_v, w_o, sink,
    )


def solution(mesh):
    in_specs = (
        P(("sp", "tp"), None), P("sp", None), P(), P(), P("sp", "tp"), P("sp", "tp"), P("sp", "tp"),
        P(None, "tp"), P(None, "tp"), P(None, "tp"), P("tp", None), P(),
    )
    return jax.shard_map(
        shards, mesh=mesh, in_specs=in_specs, out_specs=P(("sp", "tp"), None), check_vma=False
    )
```
